32 devices in a mesh: grp: 2 (over x), sp: 4 (over z), tp: 4 (over y, core).
Axes of the slice: x: 2, y: 2, z: 4, core: 2. Of those that a mesh axis runs over, the one named last changes fastest.
Arguments:
- tokens: bfloat16 [1792, 4096], P(('grp', 'sp'), 'tp'), parts along dimension 0, may hold values from -130 to 130
- rms_gain: float32 [2, 4096], replicated, may hold values from 0.1 to 1.9
- w_value: bfloat16 [2, 4096, 2048], P(None, 'sp', 'tp'), may hold values from -0.09375 to 0.09375
- w_gate: bfloat16 [2, 4096, 2048], P(None, 'sp', 'tp'), may hold values from -0.09375 to 0.09375
- taps: float32 [2, 31, 2048], P(None, None, 'tp'), may hold values from -8 to 8
- ln_gain: float32 [2, 2048], P(None, 'tp'), may hold values from 0.1 to 1.9
- ln_bias: float32 [2, 2048], P(None, 'tp'), may hold values from -3 to 3
- w_out: bfloat16 [2, 2048, 4096], P(None, 'sp', 'tp'), may hold values from -0.125 to 0.125
Outputs:
- result: bfloat16 [1792, 4096], P(('grp', 'sp'), 'tp'), parts along dimension 0
The draws below stay inside these ranges and needn't reach their ends.
There are 2 independent parts, one for each index of `grp`. The reference program is written for one: setup_inputs(seed, part) draws one part's arguments, and reference() takes and returns one part's arrays. A program takes and returns all parts, laid end to end along the dimension named above; an argument that names none is the same for every part. Nothing has to cross between parts.
All inputs are finite; a program needn't handle non-finite values.
Results may differ from the reference program's by a relative error of at most 0.009.
Values may be sent and summed in bfloat16 or wider, within the bound.
A program may use at most 64 MiB of HBM per device.

```python
import jax
import jax.numpy as jnp
from jax import lax

D = 4096
CH = 2048
WIDTH = 31
LAYERS = 2
TOKENS = 896


def draw_tokens(key, part):
    keys = jax.random.split(jax.random.fold_in(key, 11), 3)
    column = jnp.arange(D, dtype=jnp.float32) / D
    col_scale = jnp.exp(jnp.log(4.0) * column + jax.random.uniform(keys[1], (D,), jnp.float32, -0.4, 0.4))
    row_scale = jnp.exp(jax.random.uniform(keys[2], (TOKENS, 1), jnp.float32, jnp.log(0.5), jnp.log(5.0)))
    base = jax.random.truncated_normal(keys[0], -4.0, 4.0, (TOKENS, D), jnp.float32)
    return (base * col_scale[None, :] * row_scale).astype(jnp.bfloat16)


def draw_taps(key, part):
    keys = jax.random.split(jax.random.fold_in(key, 23), 2)
    channel = jnp.arange(CH, dtype=jnp.float32) / CH
    scale = jnp.exp(jnp.log(10.0) * channel[None, None, :] + jax.random.uniform(keys[1], (LAYERS, 1, CH), jnp.float32, -0.3, 0.3)) / jnp.sqrt(1.0 * WIDTH)
    base = jax.random.truncated_normal(keys[0], -3.0, 3.0, (LAYERS, WIDTH, CH), jnp.float32)
    return base * scale


def level_of(key, shape, cuts, least, top_value):
    def one(dim, parts):
        draws = jax.random.uniform(jax.random.fold_in(jax.random.fold_in(key, 6), dim), (parts,), jnp.float32, least / len(cuts), top_value / len(cuts))
        return jnp.repeat(jnp.exp(draws), shape[dim] // parts).reshape((-1,) + (1,) * (len(shape) - dim - 1))

    loudness = one(*cuts[0])
    for cut in cuts[1:]:
        loudness = loudness * one(*cut)
    return loudness


def scatter_about(own_key, shape, width, reach, shards=(), kind=jnp.bfloat16):
    array = width * jax.random.normal(own_key, shape, jnp.float32)
    if shards:
        array = array * level_of(own_key, shape, shards, -0.22, 0.18)
    return jnp.clip(array, -reach, reach).astype(kind)


def setup_inputs(seed: int = 0, part: int = 0) -> dict:
    arg_keys = jax.random.split(jax.random.key(seed), 9)
    part_keys = jax.random.split(jax.random.fold_in(arg_keys[8], part), 9)
    tokens = draw_tokens(jax.random.fold_in(jax.random.fold_in(arg_keys[8], part), 71), part)
    rms_gain = jnp.clip(1.0 + 0.18 * jax.random.normal(arg_keys[1], (LAYERS, D), jnp.float32), 0.1, 1.9)
    w_value = scatter_about(arg_keys[2], (LAYERS, D, CH), D ** -0.5, 0.09375, ((1, 4), (2, 4)))
    w_gate = scatter_about(arg_keys[3], (LAYERS, D, CH), D ** -0.5, 0.09375, ((1, 4), (2, 4)))
    taps = draw_taps(jax.random.fold_in(arg_keys[8], 71), part)
    ln_gain = jnp.clip(1.0 + 0.18 * jax.random.normal(arg_keys[5], (LAYERS, CH), jnp.float32), 0.1, 1.9)
    ln_bias = scatter_about(arg_keys[6], (LAYERS, CH), 0.5, 3.0, ((1, 4),), jnp.float32)
    w_out = scatter_about(arg_keys[7], (LAYERS, CH, D), CH ** -0.5, 0.125, ((1, 4), (2, 4)))
    return dict(tokens=tokens, rms_gain=rms_gain, w_value=w_value, w_gate=w_gate, taps=taps, ln_gain=ln_gain, ln_bias=ln_bias, w_out=w_out)


def reference(tokens, rms_gain, w_value, w_gate, taps, ln_gain, ln_bias, w_out):
    hidden = tokens
    for layer in range(LAYERS):
        wide = hidden.astype(jnp.float32)
        normed = (wide * lax.rsqrt(lax.optimization_barrier(jnp.mean(wide * wide, axis=1, keepdims=True)) + 1e-06) * rms_gain[layer]).astype(jnp.bfloat16)
        value = jnp.dot(normed, w_value[layer], preferred_element_type=jnp.float32)
        gate = jnp.dot(normed, w_gate[layer], preferred_element_type=jnp.float32)
        glu = (value * jax.nn.sigmoid(gate)).astype(jnp.bfloat16)
        padded = jnp.concatenate([jnp.zeros((WIDTH - 1, CH), jnp.bfloat16), glu], axis=0).astype(jnp.float32)
        conv = jnp.zeros((TOKENS, CH), jnp.float32)
        for k in range(WIDTH):
            conv = conv + taps[layer, k][None, :] * padded[k:k + TOKENS]
        mean = lax.optimization_barrier(jnp.mean(conv, axis=1, keepdims=True))
        var = lax.optimization_barrier(jnp.mean(conv * conv, axis=1, keepdims=True)) - mean * mean
        normed_conv = (conv - mean) * lax.rsqrt(var + 1e-05) * ln_gain[layer] + ln_bias[layer]
        act = jax.nn.silu(normed_conv).astype(jnp.bfloat16)
        branch = jnp.dot(act, w_out[layer], preferred_element_type=jnp.float32)
        hidden = (hidden.astype(jnp.float32) + branch).astype(jnp.bfloat16)
    return hidden
```

```python
import jax
import jax.numpy as jnp
from jax import lax
from jax.sharding import PartitionSpec as P


def passed_along(block, axis, distance):
    devices = range(lax.axis_size(axis))
    route = [(i - distance, i) for i in devices if i - distance in devices]
    return lax.ppermute(block, axis, route)


def norm_rows(wide, gain):
    return (wide * lax.rsqrt(jnp.mean(wide * wide, axis=1, keepdims=True) + 1e-06) * gain).astype(
        jnp.bfloat16
    )


def to_depth(rows):
    return lax.all_to_all(rows, "sp", split_axis=1, concat_axis=0, tiled=True)


def summed(partial):
    sp = lax.axis_size("sp")
    rows = partial.shape[0] // sp
    parts = partial.astype(jnp.bfloat16).reshape(sp, rows, partial.shape[1])
    parts = lax.all_to_all(parts, "sp", split_axis=0, concat_axis=0, tiled=True)
    return jnp.sum(parts.astype(jnp.float32), axis=0)


def shards(tokens, rms_gain, w_value, w_gate, taps, ln_gain, ln_bias, w_out):
    layers = w_value.shape[0]
    tok_rows = tokens.shape[0]
    chans = w_value.shape[2]
    all_chans = chans * lax.axis_size("tp")
    reach = taps.shape[1]
    current = tokens
    for layer in range(layers):
        whole_rows = lax.all_gather(current, "tp", axis=1, tiled=True)
        normed = to_depth(norm_rows(whole_rows.astype(jnp.float32), rms_gain[layer]))
        both = jnp.concatenate([w_value[layer], w_gate[layer]], axis=1)
        both = summed(jnp.dot(normed, both, preferred_element_type=jnp.float32))
        glu = (both[:, :chans] * jax.nn.sigmoid(both[:, chans:])).astype(jnp.bfloat16)
        earlier = passed_along(glu[tok_rows - (reach - 1) :], "sp", 1)
        extended = jnp.concatenate([earlier, glu], axis=0).astype(jnp.float32)
        conv = jnp.zeros((tok_rows, chans), jnp.float32)
        for k in range(reach):
            conv = conv + taps[layer, k][None, :] * extended[k : k + tok_rows]
        total, total_sq = lax.psum((jnp.sum(conv, axis=1), jnp.sum(conv * conv, axis=1)), "tp")
        mean = total / all_chans
        var = total_sq / all_chans - mean * mean
        shaped = (conv - mean[:, None]) * lax.rsqrt(var + 1e-05)[:, None] * ln_gain[layer][
            None, :
        ] + ln_bias[layer][None, :]
        act = jax.nn.silu(shaped).astype(jnp.bfloat16)
        act_all = to_depth(lax.all_gather(act, "tp", axis=1, tiled=True))
        branch = summed(jnp.dot(act_all, w_out[layer], preferred_element_type=jnp.float32))
        current = (current.astype(jnp.float32) + branch).astype(jnp.bfloat16)
    return current


def solution(mesh):
    return jax.shard_map(
        shards,
        mesh=mesh,
        in_specs=(
            P(("grp", "sp"), "tp"),
            P(),
            P(None, "sp", "tp"),
            P(None, "sp", "tp"),
            P(None, None, "tp"),
            P(None, "tp"),
            P(None, "tp"),
            P(None, "sp", "tp"),
        ),
        out_specs=P(("grp", "sp"), "tp"),
        check_vma=False,
    )
```

```python
import functools

import jax
import jax.numpy as jnp
from jax import lax
from jax.experimental import pallas as pl
from jax.experimental.pallas import tpu as pltpu
from jax.sharding import PartitionSpec as P

LANES = 128
BF16, F32 = jnp.bfloat16, jnp.float32


def passed_along(block, axis, distance):
    devices = range(lax.axis_size(axis))
    route = [(i - distance, i) for i in devices if i - distance in devices]
    return lax.ppermute(block, axis, route)


def norm_rows(wide, gain):
    return (wide * lax.rsqrt(jnp.mean(wide * wide, axis=1, keepdims=True) + 1e-06) * gain).astype(
        jnp.bfloat16
    )


def to_depth(rows):
    return lax.all_to_all(rows, "sp", split_axis=1, concat_axis=0, tiled=True)


def summed(partial):
    sp = lax.axis_size("sp")
    rows = partial.shape[0] // sp
    parts = partial.astype(jnp.bfloat16).reshape(sp, rows, partial.shape[1])
    parts = lax.all_to_all(parts, "sp", split_axis=0, concat_axis=0, tiled=True)
    return jnp.sum(parts.astype(jnp.float32), axis=0)


def send(src, dst, send_sem, recv_sem, **where):
    return pltpu.make_async_remote_copy(
        src_ref=src,
        dst_ref=dst,
        send_sem=send_sem,
        recv_sem=recv_sem,
        device_id=where,
        device_id_type=pl.DeviceIdType.MESH,
    )


def gated_conv(
    layer, sp, tp,
    h_ref, gain_ref, wv_hbm, wg_hbm, taps_ref, lng_ref, lnb_ref, out_ref,
    wv, wg, pieces, spread, xs, going, coming, own, sq, stat, halo_out, halo_in, ext, conv, acts,
    w_sem, a_send, a_recv, b_send, c_send, c_relay, x_recv, r_send, r_recv,
    q_send, q_recv, s_send, s_recv, h_send, h_recv, g_send, g_relay, g_recv,
):
    s, c = lax.axis_index("sp"), lax.axis_index("tp")
    rows, depth = h_ref.shape
    chans = taps_ref.shape[2]
    part = depth // tp
    step = going.shape[-1]
    chunks = chans // step
    pairs = tp // 2
    sibling = c + 1 - 2 * (c % 2)
    reach = taps_ref.shape[1]
    pad = halo_in.shape[0]

    loads = [
        pltpu.make_async_copy(wv_hbm.at[layer], wv, w_sem.at[0]),
        pltpu.make_async_copy(wg_hbm.at[layer], wg, w_sem.at[1]),
    ]
    for load in loads:
        load.start()

    barrier = pltpu.get_barrier_semaphore()
    for j in range(1, tp):
        pl.semaphore_signal(
            barrier, inc=1, device_id={"tp": (c + j) % tp}, device_id_type=pl.DeviceIdType.MESH
        )
    for j in range(1, sp):
        pl.semaphore_signal(
            barrier, inc=1, device_id={"sp": (s + j) % sp}, device_id_type=pl.DeviceIdType.MESH
        )

    total = jnp.zeros((rows, LANES), F32)
    for p in range(tp):
        for lane in range(0, part, LANES):
            at = p * part + lane
            wide = h_ref[:, at : at + LANES].astype(F32)
            total = total + wide * wide
            pieces[p, :, lane : lane + LANES] = (
                wide * gain_ref[0:1, at : at + LANES]
            ).astype(BF16)
    sq[c] = total
    spread[c] = pieces[c]
    pl.semaphore_wait(barrier, tp + sp - 2)

    def a_copy(to, frm):
        return send(pieces.at[to], spread.at[frm], a_send.at[to], a_recv.at[frm], tp=to)

    def q_copy(to, frm):
        return send(sq.at[frm], sq.at[frm], q_send.at[to], q_recv.at[frm], tp=to)

    for j in range(1, tp):
        a_copy((c + j) % tp, c).start()
    for j in range(1, tp):
        q_copy((c + j) % tp, c).start()

    def b_copy(to, frm):
        return send(spread.at[to], xs.at[c, frm], b_send.at[to], x_recv.at[c, frm], sp=to)

    for j in range(1, sp + 1):
        to = (s + j) % sp

        @pl.when(to != c)
        def _():
            a_copy(c, to).wait_recv()

        if j < sp:
            b_copy(to, s).start()
    xs[c, s] = spread[s]

    def c_copy(to, d, sem):
        return send(xs.at[c, d], xs.at[c, d], sem, x_recv.at[c, d], tp=to)

    def relay(p, d):
        return send(xs.at[p, d], xs.at[p, d], c_relay.at[p, d], x_recv.at[p, d], tp=sibling)

    def arrived(p, d):
        send(xs.at[p, d], xs.at[p, d], c_relay.at[p, d], x_recv.at[p, d], tp=sibling).wait_recv()

    def gather(d):
        @pl.when(d != s)
        def _():
            arrived(c, d)

        for j in range(1, pairs):
            c_copy((c + 2 * j) % tp, d, c_send.at[j, d]).start()
        c_copy(sibling, d, c_send.at[0, d]).start()

    def place(j):
        left = j % 2
        k = j // 2
        d = (1 - left) * (sp - 1 - k) + left * k
        return left, d, (1 - 2 * left) * (d - s) > 0

    def each(body):
        def one(j, carry):
            left, d, valid = place(j)

            @pl.when(valid)
            def _():
                body(left, d)

            return carry

        lax.fori_loop(0, 2 * (sp - 1), one, 0)

    each(lambda left, d: gather(d))
    gather(s)
    for load in loads:
        load.wait()

    def ready(d):
        for j in range(1, pairs):
            p = (c + 2 * j) % tp
            arrived(p, d)
            relay(p, d).start()
        for j in range(pairs):
            arrived((sibling + 2 * j) % tp, d)

    def product(d, weight, at):
        acc = jnp.zeros((rows, step), F32)
        for p in range(tp):
            acc = acc + jnp.dot(
                xs[p, d],
                weight[p * part : (p + 1) * part, pl.ds(at, step)],
                preferred_element_type=F32,
            )
        return acc

    def r_copy(left, d, slot):
        return send(
            going.at[left, d, slot],
            coming.at[left, d, slot],
            r_send.at[left, d, slot],
            r_recv.at[left, d, slot],
            sp=s + 1 - 2 * left,
        )

    def r_arrived(left, d, slot):
        send(
            going.at[left, d, slot],
            coming.at[left, d, slot],
            r_send.at[left, d, slot],
            r_recv.at[left, d, slot],
            sp=(s + 1) % sp,
        ).wait_recv()

    def upstream(left):
        return (1 - left) * s + left * (sp - 1 - s) > 0

    def partial(left, d):
        ready(d)
        for half, weight in enumerate((wv, wg)):

            def one(i, carry):
                slot = half * chunks + i
                own[half] = product(d, weight, pl.multiple_of(i * step, step))

                @pl.when(upstream(left))
                def _():
                    r_arrived(left, d, slot)
                    own[half] += coming[left, d, slot].astype(F32)

                going[left, d, slot] = own[half].astype(BF16)
                r_copy(left, d, slot).start()
                return carry

            lax.fori_loop(0, chunks, one, 0)

    each(partial)

    ready(s)
    for j in range(1, tp):
        q_copy(c, (c + j) % tp).wait_recv()
    squares = sq[0]
    for p in range(1, tp):
        squares = squares + sq[p]
    scale = lax.rsqrt(jnp.sum(squares, axis=1, keepdims=True) / (depth * tp) + 1e-06)

    def finish(i, carry):
        at = pl.multiple_of(i * step, step)
        for half, weight in enumerate((wv, wg)):
            slot = half * chunks + i
            own[half] = product(s, weight, at)
            for left in range(2):

                @pl.when(upstream(left))
                def _():
                    r_arrived(left, s, slot)
                    own[half] += coming[left, s, slot].astype(F32)

        glu = (own[0] * scale * jax.nn.sigmoid(own[1] * scale)).astype(BF16)
        ext[pad:, pl.ds(at, step)] = glu.astype(F32)
        halo_out[:, pl.ds(at, step)] = glu[rows - pad :]
        return carry

    lax.fori_loop(0, chunks, finish, 0)

    def h_copy(to):
        return send(halo_out, halo_in, h_send, h_recv, sp=to)

    @pl.when(s < sp - 1)
    def _():
        h_copy(s + 1).start()

    @pl.when(s > 0)
    def _():
        h_copy((s + 1) % sp).wait_recv()
        ext[:pad] = halo_in[...].astype(F32)

    @pl.when(s == 0)
    def _():
        ext[:pad] = jnp.zeros((pad, chans), F32)

    first = pad - (reach - 1)

    def convolve(i, carry):
        lanes = pl.ds(pl.multiple_of(i * LANES, LANES), LANES)
        acc = jnp.zeros((rows, LANES), F32)
        for k in range(reach):
            acc = acc + taps_ref[0, k : k + 1, lanes] * ext[first + k : first + k + rows, lanes]
        conv[:, lanes] = acc
        return carry

    lax.fori_loop(0, chans // LANES, convolve, 0)
    whole = conv[...]
    lane = lax.broadcasted_iota(jnp.int32, (rows, LANES), 1)
    stat[c] = jnp.where(
        lane == 0,
        jnp.sum(whole, axis=1, keepdims=True),
        jnp.sum(whole * whole, axis=1, keepdims=True),
    )

    def s_copy(to, frm):
        return send(stat.at[frm], stat.at[frm], s_send.at[to], s_recv.at[frm], tp=to)

    for j in range(1, tp):
        s_copy((c + j) % tp, c).start()
    for j in range(1, tp):
        s_copy(c, (c + j) % tp).wait_recv()
    stats = stat[0]
    for p in range(1, tp):
        stats = stats + stat[p]
    mean = stats[:, 0:1] / (chans * tp)
    var = stats[:, 1:2] / (chans * tp) - mean * mean
    inv = lax.rsqrt(var + 1e-05)
    for at in range(0, chans, LANES):
        lanes = slice(at, at + LANES)
        shaped = (conv[:, lanes] - mean) * inv * lng_ref[0:1, lanes] + lnb_ref[0:1, lanes]
        acts[c, :, lanes] = (shaped / (1.0 + jnp.exp(-shaped))).astype(BF16)

    def g_copy(to, p, sem):
        return send(acts.at[p], acts.at[p], sem, g_recv.at[p], tp=to)

    for j in range(1, pairs):
        g_copy((c + 2 * j) % tp, c, g_send.at[j]).start()
    g_copy(sibling, c, g_send.at[0]).start()
    for j in range(1, pairs):
        p = (c + 2 * j) % tp
        g_copy(sibling, p, g_relay.at[p]).wait_recv()
        g_copy(sibling, p, g_relay.at[p]).start()
    for j in range(pairs):
        p = (sibling + 2 * j) % tp
        g_copy(sibling, p, g_relay.at[p]).wait_recv()
    cut = out_ref.shape[3]
    for p in range(tp):
        for n in range(chans // cut):
            out_ref[n, p] = acts[p, :, n * cut : (n + 1) * cut]

    for j in range(1, tp):
        a_copy((c + j) % tp, c).wait_send()
        q_copy((c + j) % tp, c).wait_send()
        s_copy((c + j) % tp, c).wait_send()
    for j in range(1, sp):
        b_copy((s + j) % sp, s).wait_send()

    def sent(d, carry):
        c_copy(sibling, d, c_send.at[0, d]).wait_send()
        for j in range(1, pairs):
            p = (c + 2 * j) % tp
            c_copy(p, d, c_send.at[j, d]).wait_send()
            relay(p, d).wait_send()
        return carry

    lax.fori_loop(0, sp, sent, 0)

    def partial_sent(left, d):
        def one(slot, carry):
            r_copy(left, d, slot).wait_send()
            return carry

        lax.fori_loop(0, 2 * chunks, one, 0)

    each(partial_sent)

    @pl.when(s < sp - 1)
    def _():
        h_copy(s + 1).wait_send()

    g_copy(sibling, c, g_send.at[0]).wait_send()
    for j in range(1, pairs):
        p = (c + 2 * j) % tp
        g_copy(p, c, g_send.at[j]).wait_send()
        g_copy(sibling, p, g_relay.at[p]).wait_send()


def fused_branch(layer, cuts, h, gain, w_value, w_gate, taps, ln_gain, ln_bias):
    sp, tp = lax.axis_size("sp"), lax.axis_size("tp")
    rows, depth = h.shape
    chans, reach = w_value.shape[2], taps.shape[1]
    part, step = depth // tp, min(2 * LANES, chans)
    slots = 2 * (chans // step)
    pad = -(-(reach - 1) // 16) * 16
    vmem, dma = pltpu.VMEM, pltpu.SemaphoreType.DMA
    here = pl.BlockSpec(memory_space=pltpu.VMEM)
    there = pl.BlockSpec(memory_space=pl.ANY)
    return pl.pallas_call(
        functools.partial(gated_conv, layer, sp, tp),
        out_shape=jax.ShapeDtypeStruct((cuts, tp, rows, chans // cuts), BF16),
        in_specs=[here, here, there, there, here, here, here],
        out_specs=here,
        scratch_shapes=[
            vmem((depth, chans), BF16),
            vmem((depth, chans), BF16),
            vmem((tp, rows, part), BF16),
            vmem((tp, rows, part), BF16),
            vmem((tp, sp, rows, part), BF16),
            vmem((2, sp, slots, rows, step), BF16),
            vmem((2, sp, slots, rows, step), BF16),
            vmem((2, rows, step), F32),
            vmem((tp, rows, LANES), F32),
            vmem((tp, rows, LANES), F32),
            vmem((pad, chans), BF16),
            vmem((pad, chans), BF16),
            vmem((pad + rows, chans), F32),
            vmem((rows, chans), F32),
            vmem((tp, rows, chans), BF16),
            dma((2,)), dma((tp,)), dma((tp,)), dma((sp,)), dma((tp, sp)), dma((tp, sp)),
            dma((tp, sp)), dma((2, sp, slots)), dma((2, sp, slots)),
            dma((tp,)), dma((tp,)), dma((tp,)), dma((tp,)), dma, dma,
            dma((tp,)), dma((tp,)), dma((tp,)),
        ],
        compiler_params=pltpu.CompilerParams(
            collective_id=layer, has_side_effects=True, vmem_limit_bytes=48 * 2**20
        ),
        cost_estimate=pl.CostEstimate(
            flops=120_000_000_000, bytes_accessed=200_000_000, transcendentals=0
        ),
    )(h, gain, w_value, w_gate, taps, ln_gain, ln_bias)


def gathered(weight):
    grp = lax.axis_size("grp")
    share = weight.shape[0] // grp
    mine = lax.dynamic_slice_in_dim(weight, lax.axis_index("grp") * share, share, 0)
    mine = lax.all_gather(mine, "sp", axis=0, tiled=True)
    return lax.all_gather(mine, "grp", axis=0, tiled=True)


def fits(tokens, w_value, taps):
    sp, tp, grp = (lax.axis_size(a) for a in ("sp", "tp", "grp"))
    rows, depth = tokens.shape
    chans = w_value.shape[2]
    return (
        sp == tp
        and tp % 2 == 0
        and depth % (tp * LANES) == 0
        and chans % (LANES * grp) == 0
        and chans % min(2 * LANES, chans) == 0
        and rows % 16 == 0
        and rows >= -(-(taps.shape[1] - 1) // 16) * 16
    )


def fused(tokens, rms_gain, w_value, w_gate, taps, ln_gain, ln_bias, w_out):
    grp = lax.axis_size("grp")
    rows, depth = tokens.shape
    gains = lax.dynamic_slice_in_dim(rms_gain, lax.axis_index("tp") * depth, depth, 1)
    current = tokens
    weights = [gathered(w_out[layer]) for layer in range(w_value.shape[0])]
    for layer, weight in enumerate(weights):
        one = slice(layer, layer + 1)
        act = fused_branch(
            layer, grp, current, gains[one], w_value, w_gate, taps[one], ln_gain[one], ln_bias[one]
        )
        act = act.transpose(2, 0, 1, 3).reshape(rows, -1)
        branch = jnp.dot(act, weight, preferred_element_type=F32)
        current = (current.astype(F32) + branch).astype(BF16)
    return current


def shards(tokens, rms_gain, w_value, w_gate, taps, ln_gain, ln_bias, w_out):
    if fits(tokens, w_value, taps):
        return fused(tokens, rms_gain, w_value, w_gate, taps, ln_gain, ln_bias, w_out)
    layers = w_value.shape[0]
    tok_rows = tokens.shape[0]
    chans = w_value.shape[2]
    all_chans = chans * lax.axis_size("tp")
    reach = taps.shape[1]
    current = tokens
    for layer in range(layers):
        whole_rows = lax.all_gather(current, "tp", axis=1, tiled=True)
        normed = to_depth(norm_rows(whole_rows.astype(jnp.float32), rms_gain[layer]))
        both = jnp.concatenate([w_value[layer], w_gate[layer]], axis=1)
        both = summed(jnp.dot(normed, both, preferred_element_type=jnp.float32))
        glu = (both[:, :chans] * jax.nn.sigmoid(both[:, chans:])).astype(jnp.bfloat16)
        earlier = passed_along(glu[tok_rows - (reach - 1) :], "sp", 1)
        extended = jnp.concatenate([earlier, glu], axis=0).astype(jnp.float32)
        conv = jnp.zeros((tok_rows, chans), jnp.float32)
        for k in range(reach):
            conv = conv + taps[layer, k][None, :] * extended[k : k + tok_rows]
        total, total_sq = lax.psum((jnp.sum(conv, axis=1), jnp.sum(conv * conv, axis=1)), "tp")
        mean = total / all_chans
        var = total_sq / all_chans - mean * mean
        shaped = (conv - mean[:, None]) * lax.rsqrt(var + 1e-05)[:, None] * ln_gain[layer][
            None, :
        ] + ln_bias[layer][None, :]
        act = jax.nn.silu(shaped).astype(jnp.bfloat16)
        act_all = to_depth(lax.all_gather(act, "tp", axis=1, tiled=True))
        branch = summed(jnp.dot(act_all, w_out[layer], preferred_element_type=jnp.float32))
        current = (current.astype(jnp.float32) + branch).astype(jnp.bfloat16)
    return current


def solution(mesh):
    return jax.shard_map(
        shards,
        mesh=mesh,
        in_specs=(
            P(("grp", "sp"), "tp"),
            P(),
            P(None, "sp", "tp"),
            P(None, "sp", "tp"),
            P(None, None, "tp"),
            P(None, "tp"),
            P(None, "tp"),
            P(None, "sp", "tp"),
        ),
        out_specs=P(("grp", "sp"), "tp"),
        check_vma=False,
    )
```

```python
import functools

import jax
import jax.numpy as jnp
from jax import lax
from jax.experimental import pallas as pl
from jax.experimental.pallas import tpu as pltpu
from jax.sharding import PartitionSpec as P

LANES = 128
BF16, F32 = jnp.bfloat16, jnp.float32


def passed_along(block, axis, distance):
    devices = range(lax.axis_size(axis))
    route = [(i - distance, i) for i in devices if i - distance in devices]
    return lax.ppermute(block, axis, route)


def norm_rows(wide, gain):
    return (wide * lax.rsqrt(jnp.mean(wide * wide, axis=1, keepdims=True) + 1e-06) * gain).astype(
        jnp.bfloat16
    )


def to_depth(rows):
    return lax.all_to_all(rows, "sp", split_axis=1, concat_axis=0, tiled=True)


def summed(partial):
    sp = lax.axis_size("sp")
    rows = partial.shape[0] // sp
    parts = partial.astype(jnp.bfloat16).reshape(sp, rows, partial.shape[1])
    parts = lax.all_to_all(parts, "sp", split_axis=0, concat_axis=0, tiled=True)
    return jnp.sum(parts.astype(jnp.float32), axis=0)


def send(src, dst, send_sem, recv_sem, **where):
    return pltpu.make_async_remote_copy(
        src_ref=src,
        dst_ref=dst,
        send_sem=send_sem,
        recv_sem=recv_sem,
        device_id=where,
        device_id_type=pl.DeviceIdType.MESH,
    )


def gated_conv(
    layer, sp, tp,
    h_ref, gain_ref, wv_hbm, wg_hbm, taps_ref, lng_ref, lnb_ref, wo_hbm, out_ref,
    wv, wg, wo, pieces, spread, xs, going, coming, own, sq, stat, halo_out, halo_in, ext, conv, acts,
    w_sem, a_send, a_recv, b_send, c_send, c_relay, x_recv, r_send, r_recv,
    q_send, q_recv, s_send, s_recv, h_send, h_recv, g_send, g_relay, g_recv,
    o_sem, z_send, z_recv, y_send, y_recv,
):
    s, c, g = lax.axis_index("sp"), lax.axis_index("tp"), lax.axis_index("grp")
    grp, share = wo.shape[1], wo.shape[2]
    padded = sq.shape[2]
    rows, depth = h_ref.shape
    chans = taps_ref.shape[2]
    part = depth // tp
    step = going.shape[-1]
    chunks = chans // step
    pairs = tp // 2
    sibling = c + 1 - 2 * (c % 2)
    reach = taps_ref.shape[1]
    pad = halo_in.shape[0]

    loads = [
        pltpu.make_async_copy(wv_hbm.at[layer], wv, w_sem.at[0]),
        pltpu.make_async_copy(wg_hbm.at[layer], wg, w_sem.at[1]),
    ]
    for n in range(grp):
        loads.append(
            pltpu.make_async_copy(
                wo_hbm.at[layer, pl.ds(n * share, share)], wo.at[s, n], o_sem.at[n]
            )
        )
    for load in loads:
        load.start()

    barrier = pltpu.get_barrier_semaphore()
    for j in range(1, tp):
        pl.semaphore_signal(
            barrier, inc=1, device_id={"tp": (c + j) % tp}, device_id_type=pl.DeviceIdType.MESH
        )
    for j in range(1, sp):
        pl.semaphore_signal(
            barrier, inc=1, device_id={"sp": (s + j) % sp}, device_id_type=pl.DeviceIdType.MESH
        )
    for j in range(1, grp):
        pl.semaphore_signal(
            barrier, inc=1, device_id={"grp": (g + j) % grp}, device_id_type=pl.DeviceIdType.MESH
        )

    def to_row(column):
        column = jnp.concatenate([column, jnp.zeros((padded - rows, LANES), F32)], axis=0)
        return jnp.sum(column.T, axis=0, keepdims=True)

    def to_column(row):
        return jnp.broadcast_to(row, (LANES, padded)).T[:rows, 0:1]

    total = jnp.zeros((rows, LANES), F32)
    for p in range(tp):
        for lane in range(0, part, LANES):
            at = p * part + lane
            wide = h_ref[:, at : at + LANES].astype(F32)
            total = total + wide * wide
            pieces[p, :, lane : lane + LANES] = (
                wide * gain_ref[0:1, at : at + LANES]
            ).astype(BF16)
    sq[c] = jnp.broadcast_to(to_row(total), sq.shape[1:])
    spread[c] = pieces[c]
    pl.semaphore_wait(barrier, tp + sp + grp - 3)

    def a_copy(to, frm):
        return send(pieces.at[to], spread.at[frm], a_send.at[to], a_recv.at[frm], tp=to)

    def q_copy(to, frm):
        return send(sq.at[frm], sq.at[frm], q_send.at[to], q_recv.at[frm], tp=to)

    for j in range(1, tp):
        a_copy((c + j) % tp, c).start()
    for j in range(1, tp):
        q_copy((c + j) % tp, c).start()

    def z_copy(left, o):
        return send(
            wo.at[o, g], wo.at[o, g], z_send.at[left, o], z_recv.at[o], sp=s + 1 - 2 * left
        )

    def y_copy(j, o, n):
        return send(
            wo.at[o, n], wo.at[o, n], y_send.at[j, o], y_recv.at[o, n], grp=(g + j) % grp
        )

    def pass_on(i):
        for left in range(2):
            o = s + (2 * left - 1) * i

            @pl.when((o >= 0) & (o < sp))
            def _():
                send(
                    wo.at[o, g], wo.at[o, g], z_send.at[left, o], z_recv.at[o], sp=(s + 1) % sp
                ).wait_recv()

                @pl.when((1 - left) * (sp - 1 - s) + left * s > 0)
                def _():
                    z_copy(left, o).start()

                for j in range(1, grp):
                    y_copy(j, o, g).start()

    def b_copy(to, frm):
        return send(spread.at[to], xs.at[c, frm], b_send.at[to], x_recv.at[c, frm], sp=to)

    for j in range(1, sp + 1):
        to = (s + j) % sp

        @pl.when(to != c)
        def _():
            a_copy(c, to).wait_recv()

        if j < sp:
            b_copy(to, s).start()
    xs[c, s] = spread[s]

    def c_copy(to, d, sem):
        return send(xs.at[c, d], xs.at[c, d], sem, x_recv.at[c, d], tp=to)

    def relay(p, d):
        return send(xs.at[p, d], xs.at[p, d], c_relay.at[p, d], x_recv.at[p, d], tp=sibling)

    def arrived(p, d):
        send(xs.at[p, d], xs.at[p, d], c_relay.at[p, d], x_recv.at[p, d], tp=sibling).wait_recv()

    def gather(d):
        @pl.when(d != s)
        def _():
            arrived(c, d)

        for j in range(1, pairs):
            c_copy((c + 2 * j) % tp, d, c_send.at[j, d]).start()
        c_copy(sibling, d, c_send.at[0, d]).start()

    def place(j):
        left = j % 2
        k = j // 2
        d = (1 - left) * (sp - 1 - k) + left * k
        return left, d, (1 - 2 * left) * (d - s) > 0

    def each(body, between=lambda j: None):
        def one(j, carry):
            left, d, valid = place(j)
            between(j)

            @pl.when(valid)
            def _():
                body(j, left, d)

            return carry

        lax.fori_loop(0, 2 * (sp - 1), one, 0)

    each(lambda j, left, d: gather(d))
    gather(s)
    for load in loads:
        load.wait()

    @pl.when(s < sp - 1)
    def _():
        z_copy(0, s).start()

    @pl.when(s > 0)
    def _():
        z_copy(1, s).start()

    def ready(d):
        for j in range(1, pairs):
            p = (c + 2 * j) % tp
            arrived(p, d)
            relay(p, d).start()
        for j in range(pairs):
            arrived((sibling + 2 * j) % tp, d)

    def product(d, weight, at):
        acc = jnp.zeros((rows, step), F32)
        for p in range(tp):
            acc = acc + jnp.dot(
                xs[p, d],
                weight[p * part : (p + 1) * part, pl.ds(at, step)],
                preferred_element_type=F32,
            )
        return acc

    def r_copy(left, d, slot):
        return send(
            going.at[left, d, slot],
            coming.at[left, d, slot],
            r_send.at[left, d, slot],
            r_recv.at[left, d, slot],
            sp=s + 1 - 2 * left,
        )

    def r_arrived(left, d, slot):
        send(
            going.at[left, d, slot],
            coming.at[left, d, slot],
            r_send.at[left, d, slot],
            r_recv.at[left, d, slot],
            sp=(s + 1) % sp,
        ).wait_recv()

    def upstream(left):
        return (1 - left) * s + left * (sp - 1 - s) > 0

    def partial(j, left, d):
        ready(d)
        for half, weight in enumerate((wv, wg)):

            def one(i, carry):
                slot = half * chunks + i
                own[half] = product(d, weight, pl.multiple_of(i * step, step))

                @pl.when(upstream(left))
                def _():
                    r_arrived(left, d, slot)
                    own[half] += coming[left, d, slot].astype(F32)

                going[left, d, slot] = own[half].astype(BF16)
                r_copy(left, d, slot).start()
                return carry

            lax.fori_loop(0, chunks, one, 0)

    def between(j):
        for i in range(1, sp - 1):

            @pl.when(j == 2 * i)
            def _():
                pass_on(i)

    each(partial, between)
    ready(s)
    for j in range(1, tp):
        q_copy(c, (c + j) % tp).wait_recv()
    squares = sq[0]
    for p in range(1, tp):
        squares = squares + sq[p]
    scale = to_column(lax.rsqrt(squares[0:1] / (depth * tp) + 1e-06))

    def finish(i, carry):
        at = pl.multiple_of(i * step, step)
        for half, weight in enumerate((wv, wg)):
            slot = half * chunks + i
            own[half] = product(s, weight, at)
            for left in range(2):

                @pl.when(upstream(left))
                def _():
                    r_arrived(left, s, slot)
                    own[half] += coming[left, s, slot].astype(F32)

        glu = (own[0] * scale * jax.nn.sigmoid(own[1] * scale)).astype(BF16)
        ext[pad:, pl.ds(at, step)] = glu.astype(F32)
        halo_out[:, pl.ds(at, step)] = glu[rows - pad :]
        return carry

    lax.fori_loop(0, chunks, finish, 0)

    def h_copy(to):
        return send(halo_out, halo_in, h_send, h_recv, sp=to)

    @pl.when(s < sp - 1)
    def _():
        h_copy(s + 1).start()

    @pl.when(s > 0)
    def _():
        h_copy((s + 1) % sp).wait_recv()
        ext[:pad] = halo_in[...].astype(F32)

    @pl.when(s == 0)
    def _():
        ext[:pad] = jnp.zeros((pad, chans), F32)

    pass_on(sp - 1)
    first = pad - (reach - 1)

    def convolve(i, carry):
        lanes = pl.ds(pl.multiple_of(i * LANES, LANES), LANES)
        acc = jnp.zeros((rows, LANES), F32)
        for k in range(reach):
            acc = acc + taps_ref[0, k : k + 1, lanes] * ext[first + k : first + k + rows, lanes]
        conv[:, lanes] = acc
        return carry

    lax.fori_loop(0, chans // LANES, convolve, 0)
    total = jnp.zeros((rows, LANES), F32)
    total_sq = jnp.zeros((rows, LANES), F32)
    for at in range(0, chans, LANES):
        tile = conv[:, at : at + LANES]
        total = total + tile
        total_sq = total_sq + tile * tile
    half = sq.shape[1] // 2
    stat[c] = jnp.concatenate(
        [jnp.broadcast_to(to_row(t), (half, padded)) for t in (total, total_sq)], axis=0
    )

    def s_copy(to, frm):
        return send(stat.at[frm], stat.at[frm], s_send.at[to], s_recv.at[frm], tp=to)

    for j in range(1, tp):
        s_copy((c + j) % tp, c).start()
    for j in range(1, tp):
        s_copy(c, (c + j) % tp).wait_recv()
    stats = stat[0]
    for p in range(1, tp):
        stats = stats + stat[p]
    mean = stats[0:1] / (chans * tp)
    var = stats[half : half + 1] / (chans * tp) - mean * mean
    inv = to_column(lax.rsqrt(var + 1e-05))
    mean = to_column(mean)
    for at in range(0, chans, LANES):
        lanes = slice(at, at + LANES)
        shaped = (conv[:, lanes] - mean) * inv * lng_ref[0:1, lanes] + lnb_ref[0:1, lanes]
        acts[c, :, lanes] = (shaped / (1.0 + jnp.exp(-shaped))).astype(BF16)

    def g_copy(to, p, sem):
        return send(acts.at[p], acts.at[p], sem, g_recv.at[p], tp=to)

    for j in range(1, pairs):
        g_copy((c + 2 * j) % tp, c, g_send.at[j]).start()
    g_copy(sibling, c, g_send.at[0]).start()
    for j in range(1, pairs):
        p = (c + 2 * j) % tp
        g_copy(sibling, p, g_relay.at[p]).wait_recv()
        g_copy(sibling, p, g_relay.at[p]).start()
    for j in range(pairs):
        p = (sibling + 2 * j) % tp
        g_copy(sibling, p, g_relay.at[p]).wait_recv()
    for i in range(1, sp):
        for left in range(2):
            o = s + (2 * left - 1) * i

            @pl.when((o >= 0) & (o < sp))
            def _():
                for j in range(1, grp):
                    y_copy(j, o, (g + j) % grp).wait_recv()

    def project(i, carry):
        lanes = pl.ds(pl.multiple_of(i * step, step), step)
        acc = jnp.zeros((rows, step), F32)
        for p in range(tp):
            for n in range(grp):
                acc = acc + jnp.dot(
                    acts[p, :, n * share : (n + 1) * share],
                    wo[p, n, :, lanes],
                    preferred_element_type=F32,
                )
        out_ref[:, lanes] = (h_ref[:, lanes].astype(F32) + acc).astype(BF16)
        return carry

    lax.fori_loop(0, depth // step, project, 0)

    for j in range(1, tp):
        a_copy((c + j) % tp, c).wait_send()
        q_copy((c + j) % tp, c).wait_send()
        s_copy((c + j) % tp, c).wait_send()
    for j in range(1, sp):
        b_copy((s + j) % sp, s).wait_send()

    def sent(d, carry):
        c_copy(sibling, d, c_send.at[0, d]).wait_send()
        for j in range(1, pairs):
            p = (c + 2 * j) % tp
            c_copy(p, d, c_send.at[j, d]).wait_send()
            relay(p, d).wait_send()
        return carry

    lax.fori_loop(0, sp, sent, 0)

    def partial_sent(j, left, d):
        def one(slot, carry):
            r_copy(left, d, slot).wait_send()
            return carry

        lax.fori_loop(0, 2 * chunks, one, 0)

    each(partial_sent)

    @pl.when(s < sp - 1)
    def _():
        h_copy(s + 1).wait_send()
        z_copy(0, s).wait_send()

    @pl.when(s > 0)
    def _():
        z_copy(1, s).wait_send()

    for i in range(1, sp):
        for left in range(2):
            o = s + (2 * left - 1) * i

            @pl.when((o >= 0) & (o < sp))
            def _():
                @pl.when((1 - left) * (sp - 1 - s) + left * s > 0)
                def _():
                    z_copy(left, o).wait_send()

                for j in range(1, grp):
                    y_copy(j, o, g).wait_send()

    g_copy(sibling, c, g_send.at[0]).wait_send()
    for j in range(1, pairs):
        p = (c + 2 * j) % tp
        g_copy(p, c, g_send.at[j]).wait_send()
        g_copy(sibling, p, g_relay.at[p]).wait_send()


def fused_layer(layer, h, gain, w_value, w_gate, taps, ln_gain, ln_bias, w_out):
    sp, tp, grp = (lax.axis_size(a) for a in ("sp", "tp", "grp"))
    rows, depth = h.shape
    padded = -(-rows // LANES) * LANES
    chans, reach = w_value.shape[2], taps.shape[1]
    part, step = depth // tp, min(2 * LANES, chans)
    slots = 2 * (chans // step)
    pad = -(-(reach - 1) // 16) * 16
    vmem, dma = pltpu.VMEM, pltpu.SemaphoreType.DMA
    here = pl.BlockSpec(memory_space=pltpu.VMEM)
    there = pl.BlockSpec(memory_space=pl.ANY)
    return pl.pallas_call(
        functools.partial(gated_conv, layer, sp, tp),
        out_shape=jax.ShapeDtypeStruct((rows, depth), BF16),
        in_specs=[here, here, there, there, here, here, here, there],
        out_specs=here,
        scratch_shapes=[
            vmem((depth, chans), BF16),
            vmem((depth, chans), BF16),
            vmem((sp, grp, w_out.shape[1] // grp, depth), BF16),
            vmem((tp, rows, part), BF16),
            vmem((tp, rows, part), BF16),
            vmem((tp, sp, rows, part), BF16),
            vmem((2, sp, slots, rows, step), BF16),
            vmem((2, sp, slots, rows, step), BF16),
            vmem((2, rows, step), F32),
            vmem((tp, 8, padded), F32),
            vmem((tp, 8, padded), F32),
            vmem((pad, chans), BF16),
            vmem((pad, chans), BF16),
            vmem((pad + rows, chans), F32),
            vmem((rows, chans), F32),
            vmem((tp, rows, chans), BF16),
            dma((2,)), dma((tp,)), dma((tp,)), dma((sp,)), dma((tp, sp)), dma((tp, sp)),
            dma((tp, sp)), dma((2, sp, slots)), dma((2, sp, slots)),
            dma((tp,)), dma((tp,)), dma((tp,)), dma((tp,)), dma, dma,
            dma((tp,)), dma((tp,)), dma((tp,)),
            dma((grp,)), dma((2, sp)), dma((sp,)), dma((grp, sp)), dma((sp, grp)),
        ],
        compiler_params=pltpu.CompilerParams(
            collective_id=layer, has_side_effects=True, vmem_limit_bytes=48 * 2**20
        ),
    )(h, gain, w_value, w_gate, taps, ln_gain, ln_bias, w_out)


def fits(tokens, w_value, taps):
    sp, tp, grp = (lax.axis_size(a) for a in ("sp", "tp", "grp"))
    rows, depth = tokens.shape
    chans = w_value.shape[2]
    return (
        sp == tp
        and tp % 2 == 0
        and depth % (tp * LANES) == 0
        and chans % (LANES * grp) == 0
        and chans % min(2 * LANES, chans) == 0
        and rows % 16 == 0
        and rows >= -(-(taps.shape[1] - 1) // 16) * 16
    )


def fused(tokens, rms_gain, w_value, w_gate, taps, ln_gain, ln_bias, w_out):
    depth = tokens.shape[1]
    gains = lax.dynamic_slice_in_dim(rms_gain, lax.axis_index("tp") * depth, depth, 1)
    current = tokens
    for layer in range(w_value.shape[0]):
        one = slice(layer, layer + 1)
        current = fused_layer(
            layer, current, gains[one], w_value, w_gate, taps[one], ln_gain[one], ln_bias[one],
            w_out,
        )
    return current


def shards(tokens, rms_gain, w_value, w_gate, taps, ln_gain, ln_bias, w_out):
    if fits(tokens, w_value, taps):
        return fused(tokens, rms_gain, w_value, w_gate, taps, ln_gain, ln_bias, w_out)
    layers = w_value.shape[0]
    tok_rows = tokens.shape[0]
    chans = w_value.shape[2]
    all_chans = chans * lax.axis_size("tp")
    reach = taps.shape[1]
    current = tokens
    for layer in range(layers):
        whole_rows = lax.all_gather(current, "tp", axis=1, tiled=True)
        normed = to_depth(norm_rows(whole_rows.astype(jnp.float32), rms_gain[layer]))
        both = jnp.concatenate([w_value[layer], w_gate[layer]], axis=1)
        both = summed(jnp.dot(normed, both, preferred_element_type=jnp.float32))
        glu = (both[:, :chans] * jax.nn.sigmoid(both[:, chans:])).astype(jnp.bfloat16)
        earlier = passed_along(glu[tok_rows - (reach - 1) :], "sp", 1)
        extended = jnp.concatenate([earlier, glu], axis=0).astype(jnp.float32)
        conv = jnp.zeros((tok_rows, chans), jnp.float32)
        for k in range(reach):
            conv = conv + taps[layer, k][None, :] * extended[k : k + tok_rows]
        total, total_sq = lax.psum((jnp.sum(conv, axis=1), jnp.sum(conv * conv, axis=1)), "tp")
        mean = total / all_chans
        var = total_sq / all_chans - mean * mean
        shaped = (conv - mean[:, None]) * lax.rsqrt(var + 1e-05)[:, None] * ln_gain[layer][
            None, :
        ] + ln_bias[layer][None, :]
        act = jax.nn.silu(shaped).astype(jnp.bfloat16)
        act_all = to_depth(lax.all_gather(act, "tp", axis=1, tiled=True))
        branch = summed(jnp.dot(act_all, w_out[layer], preferred_element_type=jnp.float32))
        current = (current.astype(jnp.float32) + branch).astype(jnp.bfloat16)
    return current


def solution(mesh):
    return jax.shard_map(
        shards,
        mesh=mesh,
        in_specs=(
            P(("grp", "sp"), "tp"),
            P(),
            P(None, "sp", "tp"),
            P(None, "sp", "tp"),
            P(None, None, "tp"),
            P(None, "tp"),
            P(None, "tp"),
            P(None, "sp", "tp"),
        ),
        out_specs=P(("grp", "sp"), "tp"),
        check_vma=False,
    )
```

```python
import functools

import jax
import jax.numpy as jnp
from jax import lax
from jax.experimental import pallas as pl
from jax.experimental.pallas import tpu as pltpu
from jax.sharding import PartitionSpec as P

LANES = 128
BF16, F32 = jnp.bfloat16, jnp.float32


def passed_along(block, axis, distance):
    devices = range(lax.axis_size(axis))
    route = [(i - distance, i) for i in devices if i - distance in devices]
    return lax.ppermute(block, axis, route)


def norm_rows(wide, gain):
    return (wide * lax.rsqrt(jnp.mean(wide * wide, axis=1, keepdims=True) + 1e-06) * gain).astype(
        jnp.bfloat16
    )


def to_depth(rows):
    return lax.all_to_all(rows, "sp", split_axis=1, concat_axis=0, tiled=True)


def summed(partial):
    sp = lax.axis_size("sp")
    rows = partial.shape[0] // sp
    parts = partial.astype(jnp.bfloat16).reshape(sp, rows, partial.shape[1])
    parts = lax.all_to_all(parts, "sp", split_axis=0, concat_axis=0, tiled=True)
    return jnp.sum(parts.astype(jnp.float32), axis=0)


def send(src, dst, send_sem, recv_sem, **where):
    return pltpu.make_async_remote_copy(
        src_ref=src,
        dst_ref=dst,
        send_sem=send_sem,
        recv_sem=recv_sem,
        device_id=where,
        device_id_type=pl.DeviceIdType.MESH,
    )


def gated_conv(
    layer, sp, tp,
    h_ref, gain_ref, wv_hbm, wg_hbm, taps_ref, lng_ref, lnb_ref, wo_hbm, out_ref,
    wv, wg, wo, pieces, spread, xs, going, coming, own, sq, stat, halo_out, halo_in, ext, conv, acts,
    w_sem, a_send, a_recv, b_send, c_send, c_relay, x_recv, r_send, r_recv,
    q_send, q_recv, s_send, s_recv, h_send, h_recv, g_send, g_relay, g_recv,
    o_sem, z_send, z_recv, y_send, y_recv,
):
    s, c, g = lax.axis_index("sp"), lax.axis_index("tp"), lax.axis_index("grp")
    grp, share = wo.shape[1], wo.shape[2]
    padded = sq.shape[2]
    rows, depth = h_ref.shape
    chans = taps_ref.shape[2]
    part = depth // tp
    step = going.shape[-1]
    chunks = chans // step
    pairs = tp // 2
    sibling = c + 1 - 2 * (c % 2)
    reach = taps_ref.shape[1]
    pad = halo_in.shape[0]

    loads = [
        pltpu.make_async_copy(wv_hbm.at[layer], wv, w_sem.at[0]),
        pltpu.make_async_copy(wg_hbm.at[layer], wg, w_sem.at[1]),
    ]
    for n in range(grp):
        loads.append(
            pltpu.make_async_copy(
                wo_hbm.at[layer, pl.ds(n * share, share)], wo.at[s, n], o_sem.at[n]
            )
        )
    for load in loads:
        load.start()

    barrier = pltpu.get_barrier_semaphore()
    for j in range(1, tp):
        pl.semaphore_signal(
            barrier, inc=1, device_id={"tp": (c + j) % tp}, device_id_type=pl.DeviceIdType.MESH
        )
    for j in range(1, sp):
        pl.semaphore_signal(
            barrier, inc=1, device_id={"sp": (s + j) % sp}, device_id_type=pl.DeviceIdType.MESH
        )
    for j in range(1, grp):
        pl.semaphore_signal(
            barrier, inc=1, device_id={"grp": (g + j) % grp}, device_id_type=pl.DeviceIdType.MESH
        )

    def to_row(column):
        column = jnp.concatenate([column, jnp.zeros((padded - rows, LANES), F32)], axis=0)
        return jnp.sum(column.T, axis=0, keepdims=True)

    def to_column(row):
        return jnp.broadcast_to(row, (LANES, padded)).T[:rows, 0:1]

    total = jnp.zeros((rows, LANES), F32)
    for p in range(tp):
        for lane in range(0, part, LANES):
            at = p * part + lane
            wide = h_ref[:, at : at + LANES].astype(F32)
            total = total + wide * wide
            pieces[p, :, lane : lane + LANES] = (
                wide * gain_ref[layer : layer + 1, pl.ds(pl.multiple_of(c * depth + at, LANES), LANES)]
            ).astype(BF16)
    sq[c] = jnp.broadcast_to(to_row(total), sq.shape[1:])
    spread[c] = pieces[c]
    pl.semaphore_wait(barrier, tp + sp + grp - 3)

    def a_copy(to, frm):
        return send(pieces.at[to], spread.at[frm], a_send.at[to], a_recv.at[frm], tp=to)

    def q_copy(to, frm):
        return send(sq.at[frm], sq.at[frm], q_send.at[to], q_recv.at[frm], tp=to)

    for j in range(1, tp):
        a_copy((c + j) % tp, c).start()
    for j in range(1, tp):
        q_copy((c + j) % tp, c).start()

    def z_copy(left, o):
        return send(
            wo.at[o, g], wo.at[o, g], z_send.at[left, o], z_recv.at[o], sp=s + 1 - 2 * left
        )

    def y_copy(j, o, n):
        return send(
            wo.at[o, n], wo.at[o, n], y_send.at[j, o], y_recv.at[o, n], grp=(g + j) % grp
        )

    def pass_on(i):
        for left in range(2):
            o = s + (2 * left - 1) * i

            @pl.when((o >= 0) & (o < sp))
            def _():
                send(
                    wo.at[o, g], wo.at[o, g], z_send.at[left, o], z_recv.at[o], sp=(s + 1) % sp
                ).wait_recv()

                @pl.when((1 - left) * (sp - 1 - s) + left * s > 0)
                def _():
                    z_copy(left, o).start()

                for j in range(1, grp):
                    y_copy(j, o, g).start()

    for load in loads[2:]:
        load.wait()

    @pl.when(s < sp - 1)
    def _():
        z_copy(0, s).start()

    @pl.when(s > 0)
    def _():
        z_copy(1, s).start()

    def b_copy(to, frm):
        return send(spread.at[to], xs.at[c, frm], b_send.at[to], x_recv.at[c, frm], sp=to)

    def place(j):
        left = (j + 2 * s // sp) % 2
        k = j // 2
        d = (1 - left) * (sp - 1 - k) + left * k
        return left, d, (1 - 2 * left) * (d - s) > 0

    def each(body, between=lambda j: None):
        def one(j, carry):
            left, d, valid = place(j)
            between(j)

            @pl.when(valid)
            def _():
                body(j, left, d)

            return carry

        lax.fori_loop(0, 2 * (sp - 1), one, 0)

    def held(e):
        @pl.when(e != c)
        def _():
            a_copy(c, e).wait_recv()

    def scatter(j, left, d):
        held(d)
        b_copy(d, s).start()

    each(scatter)
    held(s)
    xs[c, s] = spread[s]

    def c_copy(to, d, sem):
        return send(xs.at[c, d], xs.at[c, d], sem, x_recv.at[c, d], tp=to)

    def relay(p, d):
        return send(xs.at[p, d], xs.at[p, d], c_relay.at[p, d], x_recv.at[p, d], tp=sibling)

    def arrived(p, d):
        send(xs.at[p, d], xs.at[p, d], c_relay.at[p, d], x_recv.at[p, d], tp=sibling).wait_recv()

    def gather(d):
        @pl.when(d != s)
        def _():
            arrived(c, d)

        for j in range(1, pairs):
            c_copy((c + 2 * j) % tp, d, c_send.at[j, d]).start()
        c_copy(sibling, d, c_send.at[0, d]).start()

    each(lambda j, left, d: gather(d))
    gather(s)
    pass_on(1)
    for load in loads[:2]:
        load.wait()

    def ready(d):
        for j in range(1, pairs):
            p = (c + 2 * j) % tp
            arrived(p, d)
            relay(p, d).start()
        for j in range(pairs):
            arrived((sibling + 2 * j) % tp, d)

    def product(d, weight, at):
        acc = jnp.zeros((rows, step), F32)
        for p in range(tp):
            acc = acc + jnp.dot(
                xs[p, d],
                weight[p * part : (p + 1) * part, pl.ds(at, step)],
                preferred_element_type=F32,
            )
        return acc

    def r_copy(left, d, slot):
        return send(
            going.at[left, d, slot],
            coming.at[left, d, slot],
            r_send.at[left, d, slot],
            r_recv.at[left, d, slot],
            sp=s + 1 - 2 * left,
        )

    def r_arrived(left, d, slot):
        send(
            going.at[left, d, slot],
            coming.at[left, d, slot],
            r_send.at[left, d, slot],
            r_recv.at[left, d, slot],
            sp=(s + 1) % sp,
        ).wait_recv()

    def upstream(left):
        return (1 - left) * s + left * (sp - 1 - s) > 0

    def partial(j, left, d):
        ready(d)
        for half, weight in enumerate((wv, wg)):

            def one(i, carry):
                slot = half * chunks + i
                own[half] = product(d, weight, pl.multiple_of(i * step, step))

                @pl.when(upstream(left))
                def _():
                    r_arrived(left, d, slot)
                    own[half] += coming[left, d, slot].astype(F32)

                going[left, d, slot] = own[half].astype(BF16)
                r_copy(left, d, slot).start()
                return carry

            lax.fori_loop(0, chunks, one, 0)

    def between(j):
        for i in range(2, sp - 1):

            @pl.when(j == 2 * i)
            def _():
                pass_on(i)

    each(partial, between)
    pass_on(sp - 1)
    ready(s)
    for j in range(1, tp):
        q_copy(c, (c + j) % tp).wait_recv()
    squares = sq[0]
    for p in range(1, tp):
        squares = squares + sq[p]
    scale = to_column(lax.rsqrt(squares[0:1] / (depth * tp) + 1e-06))

    def finish(i, carry):
        at = pl.multiple_of(i * step, step)
        for half, weight in enumerate((wv, wg)):
            slot = half * chunks + i
            own[half] = product(s, weight, at)
            for left in range(2):

                @pl.when(upstream(left))
                def _():
                    r_arrived(left, s, slot)
                    own[half] += coming[left, s, slot].astype(F32)

        glu = (own[0] * scale * jax.nn.sigmoid(own[1] * scale)).astype(BF16)
        ext[pad:, pl.ds(at, step)] = glu.astype(F32)
        halo_out[:, pl.ds(at, step)] = glu[rows - pad :]
        return carry

    lax.fori_loop(0, chunks, finish, 0)

    def h_copy(to):
        return send(halo_out, halo_in, h_send, h_recv, sp=to)

    @pl.when(s < sp - 1)
    def _():
        h_copy(s + 1).start()

    @pl.when(s > 0)
    def _():
        h_copy((s + 1) % sp).wait_recv()
        ext[:pad] = halo_in[...].astype(F32)

    @pl.when(s == 0)
    def _():
        ext[:pad] = jnp.zeros((pad, chans), F32)

    first = pad - (reach - 1)

    def convolve(i, carry):
        lanes = pl.ds(pl.multiple_of(i * LANES, LANES), LANES)
        acc = jnp.zeros((rows, LANES), F32)
        for k in range(reach):
            acc = acc + taps_ref[layer, k : k + 1, lanes] * ext[first + k : first + k + rows, lanes]
        conv[:, lanes] = acc
        return carry

    lax.fori_loop(0, chans // LANES, convolve, 0)
    total = jnp.zeros((rows, LANES), F32)
    total_sq = jnp.zeros((rows, LANES), F32)
    for at in range(0, chans, LANES):
        tile = conv[:, at : at + LANES]
        total = total + tile
        total_sq = total_sq + tile * tile
    half = sq.shape[1] // 2
    stat[c] = jnp.concatenate(
        [jnp.broadcast_to(to_row(t), (half, padded)) for t in (total, total_sq)], axis=0
    )

    def s_copy(to, frm):
        return send(stat.at[frm], stat.at[frm], s_send.at[to], s_recv.at[frm], tp=to)

    for j in range(1, tp):
        s_copy((c + j) % tp, c).start()
    for j in range(1, tp):
        s_copy(c, (c + j) % tp).wait_recv()
    stats = stat[0]
    for p in range(1, tp):
        stats = stats + stat[p]
    mean = stats[0:1] / (chans * tp)
    var = stats[half : half + 1] / (chans * tp) - mean * mean
    inv = to_column(lax.rsqrt(var + 1e-05))
    mean = to_column(mean)
    for at in range(0, chans, LANES):
        lanes = slice(at, at + LANES)
        shaped = (conv[:, lanes] - mean) * inv * lng_ref[layer : layer + 1, lanes] + lnb_ref[layer : layer + 1, lanes]
        acts[c, :, lanes] = (shaped / (1.0 + jnp.exp(-shaped))).astype(BF16)

    def g_copy(to, p, sem):
        return send(acts.at[p], acts.at[p], sem, g_recv.at[p], tp=to)

    for j in range(1, pairs):
        g_copy((c + 2 * j) % tp, c, g_send.at[j]).start()
    g_copy(sibling, c, g_send.at[0]).start()
    for j in range(1, pairs):
        p = (c + 2 * j) % tp
        g_copy(sibling, p, g_relay.at[p]).wait_recv()
        g_copy(sibling, p, g_relay.at[p]).start()
    for j in range(pairs):
        p = (sibling + 2 * j) % tp
        g_copy(sibling, p, g_relay.at[p]).wait_recv()
    for i in range(1, sp):
        for left in range(2):
            o = s + (2 * left - 1) * i

            @pl.when((o >= 0) & (o < sp))
            def _():
                for j in range(1, grp):
                    y_copy(j, o, (g + j) % grp).wait_recv()

    def project(i, carry):
        lanes = pl.ds(pl.multiple_of(i * step, step), step)
        acc = jnp.zeros((rows, step), F32)
        for p in range(tp):
            for n in range(grp):
                acc = acc + jnp.dot(
                    acts[p, :, n * share : (n + 1) * share],
                    wo[p, n, :, lanes],
                    preferred_element_type=F32,
                )
        out_ref[:, lanes] = (h_ref[:, lanes].astype(F32) + acc).astype(BF16)
        return carry

    lax.fori_loop(0, depth // step, project, 0)

    for j in range(1, tp):
        a_copy((c + j) % tp, c).wait_send()
        q_copy((c + j) % tp, c).wait_send()
        s_copy((c + j) % tp, c).wait_send()
    for j in range(1, sp):
        b_copy((s + j) % sp, s).wait_send()

    def sent(d, carry):
        c_copy(sibling, d, c_send.at[0, d]).wait_send()
        for j in range(1, pairs):
            p = (c + 2 * j) % tp
            c_copy(p, d, c_send.at[j, d]).wait_send()
            relay(p, d).wait_send()
        return carry

    lax.fori_loop(0, sp, sent, 0)

    def partial_sent(j, left, d):
        def one(slot, carry):
            r_copy(left, d, slot).wait_send()
            return carry

        lax.fori_loop(0, 2 * chunks, one, 0)

    each(partial_sent)

    @pl.when(s < sp - 1)
    def _():
        h_copy(s + 1).wait_send()
        z_copy(0, s).wait_send()

    @pl.when(s > 0)
    def _():
        z_copy(1, s).wait_send()

    for i in range(1, sp):
        for left in range(2):
            o = s + (2 * left - 1) * i

            @pl.when((o >= 0) & (o < sp))
            def _():
                @pl.when((1 - left) * (sp - 1 - s) + left * s > 0)
                def _():
                    z_copy(left, o).wait_send()

                for j in range(1, grp):
                    y_copy(j, o, g).wait_send()

    g_copy(sibling, c, g_send.at[0]).wait_send()
    for j in range(1, pairs):
        p = (c + 2 * j) % tp
        g_copy(p, c, g_send.at[j]).wait_send()
        g_copy(sibling, p, g_relay.at[p]).wait_send()


def fused_layer(layer, h, gain, w_value, w_gate, taps, ln_gain, ln_bias, w_out):
    sp, tp, grp = (lax.axis_size(a) for a in ("sp", "tp", "grp"))
    rows, depth = h.shape
    padded = -(-rows // LANES) * LANES
    chans, reach = w_value.shape[2], taps.shape[1]
    part, step = depth // tp, min(2 * LANES, chans)
    slots = 2 * (chans // step)
    pad = -(-(reach - 1) // 16) * 16
    vmem, dma = pltpu.VMEM, pltpu.SemaphoreType.DMA
    here = pl.BlockSpec(memory_space=pltpu.VMEM)
    there = pl.BlockSpec(memory_space=pl.ANY)
    return pl.pallas_call(
        functools.partial(gated_conv, layer, sp, tp),
        out_shape=jax.ShapeDtypeStruct((rows, depth), BF16),
        in_specs=[here, here, there, there, here, here, here, there],
        out_specs=here,
        scratch_shapes=[
            vmem((depth, chans), BF16),
            vmem((depth, chans), BF16),
            vmem((sp, grp, w_out.shape[1] // grp, depth), BF16),
            vmem((tp, rows, part), BF16),
            vmem((tp, rows, part), BF16),
            vmem((tp, sp, rows, part), BF16),
            vmem((2, sp, slots, rows, step), BF16),
            vmem((2, sp, slots, rows, step), BF16),
            vmem((2, rows, step), F32),
            vmem((tp, 8, padded), F32),
            vmem((tp, 8, padded), F32),
            vmem((pad, chans), BF16),
            vmem((pad, chans), BF16),
            vmem((pad + rows, chans), F32),
            vmem((rows, chans), F32),
            vmem((tp, rows, chans), BF16),
            dma((2,)), dma((tp,)), dma((tp,)), dma((sp,)), dma((tp, sp)), dma((tp, sp)),
            dma((tp, sp)), dma((2, sp, slots)), dma((2, sp, slots)),
            dma((tp,)), dma((tp,)), dma((tp,)), dma((tp,)), dma, dma,
            dma((tp,)), dma((tp,)), dma((tp,)),
            dma((grp,)), dma((2, sp)), dma((sp,)), dma((grp, sp)), dma((sp, grp)),
        ],
        compiler_params=pltpu.CompilerParams(
            collective_id=layer, has_side_effects=True, vmem_limit_bytes=48 * 2**20
        ),
    )(h, gain, w_value, w_gate, taps, ln_gain, ln_bias, w_out)


def fits(tokens, w_value, taps):
    sp, tp, grp = (lax.axis_size(a) for a in ("sp", "tp", "grp"))
    rows, depth = tokens.shape
    chans = w_value.shape[2]
    return (
        sp == tp
        and tp % 2 == 0
        and depth % (tp * LANES) == 0
        and chans % (LANES * grp) == 0
        and chans % min(2 * LANES, chans) == 0
        and rows % 16 == 0
        and rows >= -(-(taps.shape[1] - 1) // 16) * 16
    )


def fused(tokens, rms_gain, w_value, w_gate, taps, ln_gain, ln_bias, w_out):
    current = tokens
    for layer in range(w_value.shape[0]):
        current = fused_layer(
            layer, current, rms_gain, w_value, w_gate, taps, ln_gain, ln_bias, w_out
        )
    return current


def shards(tokens, rms_gain, w_value, w_gate, taps, ln_gain, ln_bias, w_out):
    if fits(tokens, w_value, taps):
        return fused(tokens, rms_gain, w_value, w_gate, taps, ln_gain, ln_bias, w_out)
    layers = w_value.shape[0]
    tok_rows = tokens.shape[0]
    chans = w_value.shape[2]
    all_chans = chans * lax.axis_size("tp")
    reach = taps.shape[1]
    current = tokens
    for layer in range(layers):
        whole_rows = lax.all_gather(current, "tp", axis=1, tiled=True)
        normed = to_depth(norm_rows(whole_rows.astype(jnp.float32), rms_gain[layer]))
        both = jnp.concatenate([w_value[layer], w_gate[layer]], axis=1)
        both = summed(jnp.dot(normed, both, preferred_element_type=jnp.float32))
        glu = (both[:, :chans] * jax.nn.sigmoid(both[:, chans:])).astype(jnp.bfloat16)
        earlier = passed_along(glu[tok_rows - (reach - 1) :], "sp", 1)
        extended = jnp.concatenate([earlier, glu], axis=0).astype(jnp.float32)
        conv = jnp.zeros((tok_rows, chans), jnp.float32)
        for k in range(reach):
            conv = conv + taps[layer, k][None, :] * extended[k : k + tok_rows]
        total, total_sq = lax.psum((jnp.sum(conv, axis=1), jnp.sum(conv * conv, axis=1)), "tp")
        mean = total / all_chans
        var = total_sq / all_chans - mean * mean
        shaped = (conv - mean[:, None]) * lax.rsqrt(var + 1e-05)[:, None] * ln_gain[layer][
            None, :
        ] + ln_bias[layer][None, :]
        act = jax.nn.silu(shaped).astype(jnp.bfloat16)
        act_all = to_depth(lax.all_gather(act, "tp", axis=1, tiled=True))
        branch = summed(jnp.dot(act_all, w_out[layer], preferred_element_type=jnp.float32))
        current = (current.astype(jnp.float32) + branch).astype(jnp.bfloat16)
    return current


def solution(mesh):
    return jax.shard_map(
        shards,
        mesh=mesh,
        in_specs=(
            P(("grp", "sp"), "tp"),
            P(),
            P(None, "sp", "tp"),
            P(None, "sp", "tp"),
            P(None, None, "tp"),
            P(None, "tp"),
            P(None, "tp"),
            P(None, "sp", "tp"),
        ),
        out_specs=P(("grp", "sp"), "tp"),
        check_vma=False,
    )
```
